32 devices in a mesh: ep: 8 (over z, y), tp: 4 (over x, core).
Axes of the slice: x: 2, y: 2, z: 4, core: 2. Of those that a mesh axis runs over, the one named last changes fastest.
Arguments:
- tokens: bfloat16 [2048, 2048], P('ep'), may hold values from -6 to 6
- cotangent: bfloat16 [2048, 2048], P('ep'), may hold values from -6 to 6
- gate_weights: bfloat16 [2048, 2], P('ep'), may hold values from 0.099609375 to 0.8984375
- routes: int32 [2048, 2], P('ep'), may hold values from 0 to 7, all different within a row; in each aligned block of 256 rows (0 to 255, 256 to 511, ...) at most 96 rows name the same one
- w_gate: bfloat16 [8, 2048, 3584], P('ep', None, 'tp'), may hold values from -0.125 to 0.125
- w_up: bfloat16 [8, 2048, 3584], P('ep', None, 'tp'), may hold values from -0.125 to 0.125
- w_down: bfloat16 [8, 3584, 2048], P('ep', 'tp'), may hold values from -0.09375 to 0.09375
Outputs:
- grad_tokens: bfloat16 [2048, 2048], P('ep', 'tp')
- grad_gates: float32 [2048, 2], P('ep')
- grad_w_gate: bfloat16 [8, 2048, 3584], P('ep', None, 'tp')
- grad_w_up: bfloat16 [8, 2048, 3584], P('ep', None, 'tp')
- grad_w_down: bfloat16 [8, 3584, 2048], P('ep', 'tp')
The draws below stay inside these ranges and needn't reach their ends.
Inputs may be any that keep to these rules, and one draw needn't show every extreme that they name: `routes`: each row names 2 different experts. Among the rows of one index of ep no expert is named by more than 96 rows, and this bound is reached in every draw.
All inputs are finite; a program needn't handle non-finite values.
Results may differ from the reference program's by a relative error of at most 0.012.
Values may be sent and summed in bfloat16 or wider, within the bound.
A program may use at most 128 MiB of HBM per device.

```python
import math
import jax
import jax.numpy as jnp
import numpy as np
from jax import lax

D = 2048
FFE = 3584
TOPK = 2
TOK_DEV = 256
EXPERTS = 8
CAP = 96
TOKENS = 2048
N_EP = 8
N_TP = 4


def levels(key, extent, cuts, low, top_value):
    loudness, own = 1.0, jax.random.fold_in(key, 6)
    for position, shards_of in cuts:
        steps = jnp.exp(jax.random.uniform(jax.random.fold_in(own, position), (shards_of,), jnp.float32, low / len(cuts), top_value / len(cuts)))
        loudness = loudness * jnp.repeat(steps, extent[position] // shards_of).reshape([-1 if axis == position else 1 for axis in range(len(extent))])
    return loudness


def routed_block(own_key, own, number, rows, number_of, top, most, lean):
    order = jax.random.permutation(own_key, number_of)
    crowded, common = load_shares(number_of, rows * top, most, lean, True), load_shares(number_of, rows * top, most, lean, False)
    places = jnp.arange(number_of)

    def named(lengths, rotation):
        used = int((lengths > 0).sum())
        fixed = max(1, used // 4)
        passed = fixed + (places - fixed + rotation * (used - fixed)) % max(1, number_of - fixed)
        return jnp.zeros((number_of,), jnp.int32).at[order[jnp.where(places < fixed, places, passed)]].set(jnp.asarray(lengths, jnp.int32))

    lengths = jnp.where(number % 4 == 0, named(crowded, number // 4), named(common, number - number // 4 - 1))
    mixed = jax.random.permutation(jax.random.fold_in(own, 3), number_of)
    giver, receiver = mixed[0:number_of // 2 * 2:2], mixed[1:number_of // 2 * 2:2]
    room = jnp.minimum(lengths[giver] - 1, most - lengths[receiver]) // 2
    room = jnp.where((giver == order[0]) | (receiver == order[0]) | (lengths[receiver] == 0), 0, jnp.maximum(room, 0))
    passed = jax.random.randint(jax.random.fold_in(own, 4), (number_of // 2,), 0, 1 << 20) % (room + 1)
    lengths = lengths.at[giver].add(-passed).at[receiver].add(passed)
    items = jnp.searchsorted(jnp.cumsum(lengths), jnp.arange(rows * top), side="right").astype(jnp.int32)
    grid = items.reshape(top, rows).T
    grid = grid[jax.random.permutation(jax.random.fold_in(own, 1), rows)]
    rotation = jax.random.randint(jax.random.fold_in(own, 2), (rows, 1), 0, top)
    return jnp.take_along_axis(grid, (jnp.arange(top)[None, :] + rotation) % top, axis=1)


def load_shares(number_of, total, bound, slope, full):
    weights = [(1 << 20) // math.isqrt(grade ** slope) + 1 for grade in range(1, number_of + 1)]
    largest = bound if full else min(bound, max(-(-total // number_of), total * weights[0] // sum(weights)))
    least = 1 if total - largest >= number_of - 1 else 0
    holding, surplus = [largest] + [least] * (number_of - 1), total - largest - least * (number_of - 1)
    while surplus > 0:
        free = [i for i in range(1, number_of) if holding[i] < largest] or [i for i in range(1, number_of) if holding[i] < bound]
        pool, left = sum([weights[i] for i in free]), surplus
        for i in free:
            addition = min(bound - holding[i], max(1, left * weights[i] // pool), surplus)
            holding[i] = holding[i] + addition
            surplus = surplus - addition
    return np.array(holding)


def scatter_about(stream_key, extent, deviation, limit, cuts=(), kind=jnp.bfloat16):
    result = deviation * jax.random.normal(stream_key, extent, jnp.float32)
    if cuts:
        result = result * levels(stream_key, extent, cuts, -0.22, 0.18)
    return jnp.clip(result, -limit, limit).astype(kind)


def setup_inputs(seed: int = 0) -> dict:
    streams_of = jax.random.split(jax.random.key(seed), 8)
    tokens = scatter_about(streams_of[0], (TOKENS, D), 1.0, 6.0, ((0, 8),))
    cotangent = scatter_about(streams_of[1], (TOKENS, D), 1.0, 6.0, ((0, 8),))
    gate_weights = jnp.clip(0.099609375 + 0.7988281 * jax.random.uniform(streams_of[2], (TOKENS, TOPK), jnp.float32) ** levels(streams_of[2], (TOKENS, TOPK), ((0, 8),), -0.2, 0.2), 0.099609375, 0.8984375).astype(jnp.bfloat16)
    routes_keys = jax.random.split(jax.random.fold_in(streams_of[3], 1), TOKENS // TOK_DEV)
    routes_turns = jax.random.permutation(jax.random.fold_in(streams_of[3], 3), TOKENS // TOK_DEV)
    routes = jax.vmap(lambda own, number: routed_block(jax.random.fold_in(streams_of[3], 2), own, number, TOK_DEV, EXPERTS, TOPK, CAP, 2))(routes_keys, routes_turns).reshape((TOKENS, TOPK))
    w_gate = scatter_about(streams_of[4], (EXPERTS, D, FFE), D ** -0.5, 0.125, ((0, 8), (2, 4)))
    w_up = scatter_about(streams_of[5], (EXPERTS, D, FFE), D ** -0.5, 0.125, ((0, 8), (2, 4)))
    w_down = scatter_about(streams_of[6], (EXPERTS, FFE, D), FFE ** -0.5, 0.09375, ((0, 8), (1, 4)))
    return dict(tokens=tokens, cotangent=cotangent, gate_weights=gate_weights, routes=routes, w_gate=w_gate, w_up=w_up, w_down=w_down)


def reference(tokens, cotangent, gate_weights, routes, w_gate, w_up, w_down):
    pair_count = TOK_DEV * TOPK
    total = TOKENS * TOPK
    routed = routes.reshape(N_EP, pair_count)
    onehot = (routed[:, :, None] == jnp.arange(EXPERTS, dtype=jnp.int32)[None, None, :]).astype(jnp.int32)
    earlier = jnp.sum((jnp.cumsum(onehot, axis=1) - onehot) * onehot, axis=2)
    source = jnp.arange(N_EP, dtype=jnp.int32)[:, None]
    slot_of = routed * (N_EP * CAP) + source * CAP + earlier
    pair_of = source * pair_count + jnp.arange(pair_count, dtype=jnp.int32)[None, :]
    slot_pair = jnp.full((EXPERTS * N_EP * CAP,), total, jnp.int32)
    slot_pair = slot_pair.at[slot_of.reshape(-1)].set(pair_of.reshape(-1)).reshape(EXPERTS, N_EP * CAP)
    tok_pad = jnp.concatenate([tokens, jnp.zeros((1, D), jnp.bfloat16)], axis=0)
    cot_pad = jnp.concatenate([cotangent, jnp.zeros((1, D), jnp.bfloat16)], axis=0)
    gate_pad = jnp.concatenate([gate_weights.reshape(-1), jnp.zeros((1,), jnp.bfloat16)], axis=0)
    block_width = FFE // N_TP

    def expert_grads(packed):
        pair_ids, weight_gate, weight_up, weight_down = packed
        token_ids = jnp.where(pair_ids < total, pair_ids // TOPK, TOKENS).astype(jnp.int32)
        x_rows = tok_pad[token_ids]
        c_rows = cot_pad[token_ids]
        weights = gate_pad[pair_ids].astype(jnp.float32)
        gate_pre = jnp.dot(x_rows, weight_gate, preferred_element_type=jnp.float32)
        up_pre = jnp.dot(x_rows, weight_up, preferred_element_type=jnp.float32)
        logistic = jax.nn.sigmoid(gate_pre)
        activated = gate_pre * logistic
        hidden = (activated * up_pre).astype(jnp.bfloat16)
        back_hidden = jnp.dot(c_rows, weight_down.T, preferred_element_type=jnp.float32)
        pair_gate = jnp.sum(hidden.astype(jnp.float32) * back_hidden, axis=1)
        scaled = (weights[:, None] * c_rows.astype(jnp.float32)).astype(jnp.bfloat16)
        grad_down = jnp.dot(hidden.T, scaled, preferred_element_type=jnp.float32).astype(jnp.bfloat16)
        grad_hidden = weights[:, None] * back_hidden
        gate_grad = (grad_hidden * up_pre * logistic * (1.0 + gate_pre * (1.0 - logistic))).astype(jnp.bfloat16)
        up_grad = (grad_hidden * activated).astype(jnp.bfloat16)
        grad_gate_w = jnp.dot(x_rows.T, gate_grad, preferred_element_type=jnp.float32).astype(jnp.bfloat16)
        grad_up_w = jnp.dot(x_rows.T, up_grad, preferred_element_type=jnp.float32).astype(jnp.bfloat16)
        summed = jnp.zeros((x_rows.shape[0], D), jnp.float32)
        for block in range(N_TP):
            lower = block * block_width
            upper = lower + block_width
            part = jnp.dot(gate_grad[:, lower:upper], weight_gate[:, lower:upper].T, preferred_element_type=jnp.float32)
            part = part + jnp.dot(up_grad[:, lower:upper], weight_up[:, lower:upper].T, preferred_element_type=jnp.float32)
            summed = summed + part.astype(jnp.bfloat16).astype(jnp.float32)
        return grad_gate_w, grad_up_w, grad_down, summed.astype(jnp.bfloat16), pair_gate

    grad_w_gate, grad_w_up, grad_w_down, pair_rows, pair_gates = lax.map(
        expert_grads, (slot_pair, w_gate, w_up, w_down))
    flat_ids = slot_pair.reshape(-1)
    pair_grad = jnp.zeros((total, D), jnp.bfloat16).at[flat_ids].set(pair_rows.reshape(-1, D), mode="drop")
    grad_tokens = jnp.sum(pair_grad.reshape(TOKENS, TOPK, D).astype(jnp.float32), axis=1).astype(jnp.bfloat16)
    grad_gates = jnp.zeros((total,), jnp.float32).at[flat_ids].set(pair_gates.reshape(-1), mode="drop")
    return grad_tokens, grad_gates.reshape(TOKENS, TOPK), grad_w_gate, grad_w_up, grad_w_down
```

```python
import functools

import jax
import jax.numpy as jnp
from jax import lax
from jax.experimental import pallas as pl
from jax.experimental.pallas import tpu as pltpu
from jax.sharding import PartitionSpec as P

MESH = pl.DeviceIdType.MESH
LAST = (((1,), (1,)), ((), ()))
FIRST = (((0,), (0,)), ((), ()))
GATE_ROWS = 16
SUM_ROWS = 8


def expert_kernel(groups, slot, quarter,
                  sent_tok, sent_cot, sent_gate, w_gate, w_up, w_down,
                  back_rows, back_gate, out_gate, out_up, out_down,
                  x_rows, c_rows, gates, wg, wu, wd, gate_pre, up_pre, back, hidden, grads,
                  part, core_got, x_got, total, gate_all, gate_sum,
                  og, ou, od,
                  load_sem, near_sem, first_send, first_recv, core_send, core_recv,
                  x_send, x_recv, second_send, second_recv, gate_send, gate_recv,
                  pair_send, pair_recv, cross_send, cross_recv, home_send, home_recv,
                  sum_send, sum_recv, sumhome_send, sumhome_recv, out_sem):
    me = lax.axis_index("ep")
    t = lax.axis_index("tp")
    core = lax.rem(t, 2)
    side = t // 2
    core_peer = side * 2 + (1 - core)
    x_peer = (1 - side) * 2 + core
    rows = groups * slot
    ffe = wg.shape[1]
    width = wg.shape[0]

    barrier = pltpu.get_barrier_semaphore()

    def greet(d, _):
        pl.semaphore_signal(barrier, inc=1, device_id=(lax.rem(me + d, groups), t),
                            device_id_type=MESH)
        return 0

    loads = [
        pltpu.make_async_copy(w_gate, wg, load_sem.at[0]),
        pltpu.make_async_copy(w_up, wu, load_sem.at[1]),
        pltpu.make_async_copy(w_down, wd, load_sem.at[2]),
    ]
    lax.fori_loop(1, groups, greet, 0)
    for o in range(1, 4):
        pl.semaphore_signal(barrier, inc=1, device_id=(me, lax.rem(t + o, 4)),
                            device_id_type=MESH)
    for load in loads:
        load.start()
    pl.semaphore_wait(barrier, groups + 2)

    def rblk(ref, s, size=slot):
        return ref.at[pl.ds(pl.multiple_of(s * size, size if size < 16 else 16), size)]

    def blk(ref, s, q):
        return ref.at[pl.ds(pl.multiple_of(s * slot, 16), slot),
                      pl.ds(pl.multiple_of(q * quarter, 128), quarter)]

    def rc(src, dst, ssem, rsem, ep, tp):
        return pltpu.make_async_remote_copy(
            src_ref=src, dst_ref=dst, send_sem=ssem, recv_sem=rsem,
            device_id=(ep, tp), device_id_type=MESH)

    def loop(lo, hi, body):
        def step(d, c):
            body(d)
            return c
        lax.fori_loop(lo, hi, step, 0)

    sent = (sent_tok, sent_cot)
    full = (x_rows, c_rows)

    def first(a, d, land):
        to = lax.rem(me + d, groups)
        return rc(rblk(sent[a], to), blk(full[a], land, t), first_send.at[a, d],
                  first_recv.at[a, d], to, t)

    def gate_copy(d, land):
        to = lax.rem(me + d, groups)
        return rc(rblk(sent_gate, to, GATE_ROWS), rblk(gates, land, GATE_ROWS),
                  gate_send.at[d], gate_recv.at[d], to, t)

    def source(d):
        return lax.rem(me - d + groups, groups)

    def to_core(a, d, q):
        s = source(d)
        return rc(blk(full[a], s, q), blk(full[a], s, q), core_send.at[a, d],
                  core_recv.at[a, d], me, core_peer)

    def to_x(a, d, q):
        s = source(d)
        return rc(blk(full[a], s, q), blk(full[a], s, q), x_send.at[a, d],
                  x_recv.at[a, d], me, x_peer)

    def to_core_again(a, d, q):
        s = source(d)
        return rc(blk(full[a], s, q), blk(full[a], s, q), second_send.at[a, d],
                  second_recv.at[a, d], me, core_peer)

    x_core_peer = (1 - side) * 2 + (1 - core)

    for a in range(2):
        loop(1, groups, lambda d, a=a: first(a, d, me).start())
        if a == 0:
            loop(1, groups, lambda d: gate_copy(d, me).start())
    near = [pltpu.make_async_copy(rblk(sent[a], me), blk(full[a], me, t), near_sem.at[a])
            for a in range(2)]
    near.append(pltpu.make_async_copy(rblk(sent_gate, me, GATE_ROWS), rblk(gates, me, GATE_ROWS),
                                      near_sem.at[2]))
    for copy in near:
        copy.start()
    for copy in near:
        copy.wait()

    def forward(a, d):
        to_x(a, d, t).start()
        to_core(a, d, t).start()

    def stage1(a, d):
        first(a, d, source(d)).wait_recv()
        forward(a, d)

    def stage2(a, d):
        to_x(a, d, x_peer).wait_recv()
        to_core_again(a, d, x_peer).start()

    def settle(a):
        def body(d):
            to_core(a, d, core_peer).wait_recv()
            to_core_again(a, d, x_core_peer).wait_recv()
        loop(0, groups, body)

    def both(a):
        def body(d):
            stage1(a, d)
            stage2(a, d - 1)
        return body

    forward(0, 0)
    loop(1, groups, both(0))
    stage2(0, groups - 1)
    forward(1, 0)
    settle(0)
    loads[0].wait()
    loads[1].wait()

    half = rows // 2
    chunks = []
    at = 0
    while at < ffe:
        chunks.append((at, min(256, ffe - at)))
        at += 256
    pieces = [(w, o, lo, n) for lo, n in chunks for w, o in ((wg, gate_pre), (wu, up_pre))]

    def product(lhs, w, o, lo, n):
        def body(h):
            r = pl.ds(pl.multiple_of(h * half, 16), half)
            o[r, lo:lo + n] = jnp.dot(lhs[r, :], w[:, lo:lo + n],
                                      preferred_element_type=jnp.float32)
        loop(0, 2, body)

    count = len(pieces)
    for i, (w, o, lo, n) in enumerate(pieces):
        product(x_rows, w, o, lo, n)
        lower, upper = max(1, i * groups // count), (i + 1) * groups // count
        if upper > lower:
            loop(lower, upper, both(1))
    stage2(1, groups - 1)
    settle(1)
    loop(1, groups, lambda d: gate_copy(d, source(d)).wait_recv())
    loads[2].wait()

    def back_product(lo, n):
        def body(h):
            r = pl.ds(pl.multiple_of(h * half, 16), half)
            back[r, lo:lo + n] = lax.dot_general(
                c_rows[r, :], wd[lo:lo + n, :], LAST, preferred_element_type=jnp.float32)
        loop(0, 2, body)

    for lo, n in chunks:
        back_product(lo, n)

    lanes = gates.shape[1]
    eye = (lax.broadcasted_iota(jnp.int32, (slot, lanes), 0)
           == lax.broadcasted_iota(jnp.int32, (slot, lanes), 1)).astype(jnp.bfloat16)

    def weight_of(s):
        g = gates[pl.ds(pl.multiple_of(s * GATE_ROWS, GATE_ROWS), GATE_ROWS), :]
        return lax.dot_general(eye, g, LAST, preferred_element_type=jnp.float32)[:, 0:1]

    def elementwise(s):
        r = pl.ds(pl.multiple_of(s * slot, 16), slot)
        weight = weight_of(s)
        summed = jnp.zeros((slot, 128), jnp.float32)
        for lo in range(0, ffe, 128):
            g = gate_pre[r, lo:lo + 128]
            u = up_pre[r, lo:lo + 128]
            b = back[r, lo:lo + 128]
            logistic = jax.nn.sigmoid(g)
            act = g * logistic
            h = (act * u).astype(jnp.bfloat16)
            hidden[r, lo:lo + 128] = h
            summed = summed + h.astype(jnp.float32) * b
            gh = weight * b
            grads[r, lo:lo + 128] = (gh * u * logistic * (1.0 + g * (1.0 - logistic))).astype(
                jnp.bfloat16)
            grads[r, ffe + lo:ffe + lo + 128] = (gh * act).astype(jnp.bfloat16)
        padded = jnp.concatenate(
            [summed, jnp.zeros((lanes - slot, 128), jnp.float32)], axis=0) if lanes > slot else summed
        row = jnp.sum(padded.T, axis=0, keepdims=True)
        gate_all[t, pl.ds(pl.multiple_of(s * SUM_ROWS, SUM_ROWS), SUM_ROWS), :] = jnp.broadcast_to(
            row, (SUM_ROWS, lanes))
        cs = c_rows[r, :].astype(jnp.float32) * weight
        c_rows[r, :] = cs.astype(jnp.bfloat16)

    def drain(a):
        def body(d):
            to_core(a, d, t).wait_send()
            to_x(a, d, t).wait_send()
            to_core_again(a, d, x_peer).wait_send()
        loop(0, groups, body)
        loop(1, groups, lambda d: first(a, d, me).wait_send())

    drain(1)
    loop(0, groups, elementwise)

    sums = [rc(gate_all.at[t], gate_all.at[t], sum_send.at[o - 1], sum_recv.at[o - 1],
               me, lax.rem(t + o, 4)) for o in range(1, 4)]
    for copy in sums:
        copy.start()

    def row_product(q, store):
        cols = pl.ds(pl.multiple_of(q * quarter, 128), quarter)

        def body(h):
            r = pl.ds(pl.multiple_of(h * half, 16), half)
            value = lax.dot_general(grads[r, 0:ffe], wg[cols, :], LAST,
                                    preferred_element_type=jnp.float32)
            value = value + lax.dot_general(grads[r, ffe:2 * ffe], wu[cols, :], LAST,
                                            preferred_element_type=jnp.float32)
            store(r, value.astype(jnp.bfloat16))
        loop(0, 2, body)

    def store_part(i):
        def store(r, value):
            part[i, r, :] = value
        return store

    pairs = [rc(part.at[i], core_got.at[i], pair_send.at[i], pair_recv.at[i], me, core_peer)
             for i in range(2)]
    row_product((1 - side) * 2 + (1 - core), store_part(0))
    pairs[0].start()
    row_product(x_peer, store_part(2))
    pairs[0].wait_recv()

    def cross(s):
        return rc(rblk(part.at[2], s), rblk(x_got, s), cross_send.at[s], cross_recv.at[s],
                  me, x_peer)

    def add_cross(d):
        s = lax.rem(me + d, groups)
        r = pl.ds(pl.multiple_of(s * slot, 16), slot)
        part[2, r, :] = (part[2, r, :].astype(jnp.float32)
                         + core_got[0, r, :].astype(jnp.float32)).astype(jnp.bfloat16)
        cross(s).start()

    loop(1, groups + 1, add_cross)
    row_product(side * 2 + (1 - core), store_part(1))
    pairs[1].start()
    row_product(t, store_part(3))
    for copy in sums:
        copy.wait_recv()
    gate_sum[...] = (gate_all[0] + gate_all[1]) + (gate_all[2] + gate_all[3])

    def sum_home(d, land):
        to = lax.rem(me + d, groups)
        return rc(rblk(gate_sum, to, SUM_ROWS), rblk(back_gate, land, SUM_ROWS),
                  sumhome_send.at[d], sumhome_recv.at[d], to, t)

    loop(1, groups, lambda d: sum_home(d, me).start())
    last = pltpu.make_async_copy(rblk(gate_sum, me, SUM_ROWS), rblk(back_gate, me, SUM_ROWS),
                                 near_sem.at[2])
    last.start()
    pairs[1].wait_recv()

    def home(d, land):
        to = lax.rem(me + d, groups)
        return rc(rblk(total, to), rblk(back_rows, land), home_send.at[d], home_recv.at[d], to, t)

    def finish(d):
        s = lax.rem(me + d, groups)
        r = pl.ds(pl.multiple_of(s * slot, 16), slot)
        cross(s).wait_recv()
        total[r, :] = (part[3, r, :].astype(jnp.float32) + core_got[1, r, :].astype(jnp.float32)
                       + x_got[r, :].astype(jnp.float32)).astype(jnp.bfloat16)

    def finish_send(d):
        finish(d)
        home(d, me).start()

    outs = []
    work = []

    def x_grad(lo, n, i):
        def run():
            left = x_rows[:, lo:lo + n]
            og[lo:lo + n, :] = lax.dot_general(
                left, grads[:, 0:ffe], FIRST, preferred_element_type=jnp.float32
            ).astype(jnp.bfloat16)
            ou[lo:lo + n, :] = lax.dot_general(
                left, grads[:, ffe:2 * ffe], FIRST, preferred_element_type=jnp.float32
            ).astype(jnp.bfloat16)
            for j, (src, dst) in enumerate(((og, out_gate), (ou, out_up))):
                copy = pltpu.make_async_copy(src.at[lo:lo + n], dst.at[lo:lo + n],
                                             out_sem.at[i, j])
                copy.start()
                outs.append(copy)
        return run

    def down_grad(lo, n, i):
        def run():
            od[lo:lo + n, :] = lax.dot_general(
                hidden[:, lo:lo + n], c_rows[...], FIRST, preferred_element_type=jnp.float32
            ).astype(jnp.bfloat16)
            copy = pltpu.make_async_copy(od.at[lo:lo + n], out_down.at[lo:lo + n],
                                         out_sem.at[i, 2])
            copy.start()
            outs.append(copy)
        return run

    step = 256
    for i, lo in enumerate(range(0, width, step)):
        work.append(x_grad(lo, min(step, width - lo), i))
    for i, (lo, n) in enumerate(chunks):
        work.append(down_grad(lo, n, i))
    lead = len(work) - 1
    for i, run in enumerate(work):
        run()
        lower, upper = max(1, 1 + i * (groups - 1) // lead), min(groups, 1 + (i + 1) * (groups - 1) // lead)
        if upper > lower:
            loop(lower, upper, finish_send)
    finish(0)
    own = pltpu.make_async_copy(rblk(total, me), rblk(back_rows, me), near_sem.at[0])
    own.start()

    loop(1, groups, lambda d: home(d, source(d)).wait_recv())
    loop(1, groups, lambda d: sum_home(d, source(d)).wait_recv())
    own.wait()
    last.wait()
    drain(0)
    loop(1, groups, lambda d: gate_copy(d, me).wait_send())
    for copy in sums + pairs:
        copy.wait_send()
    loop(0, groups, lambda s: cross(s).wait_send())
    loop(1, groups, lambda d: home(d, me).wait_send())
    loop(1, groups, lambda d: sum_home(d, me).wait_send())
    for copy in outs:
        copy.wait()


def on_device(tokens, cotangent, gate_weights, routes, w_gate, w_up, w_down):
    tok_dev, width = tokens.shape
    top_k = routes.shape[1]
    groups = lax.axis_size("ep")
    narrow = lax.axis_size("tp")
    pair_count = tok_dev * top_k
    capacity = 3 * top_k * tok_dev // (2 * groups)
    slot = -(-capacity // 16) * 16
    quarter = width // narrow
    ffe = w_gate.shape[2]
    rows = groups * slot
    lanes = -(-slot // 128) * 128
    routed = routes.reshape(pair_count)
    onehot = (routed[:, None] == jnp.arange(groups, dtype=jnp.int32)[None, :])
    before = (jnp.arange(pair_count, dtype=jnp.int32)[:, None]
              > jnp.arange(pair_count, dtype=jnp.int32)[None, :])
    counts = jnp.dot(before.astype(jnp.bfloat16), onehot.astype(jnp.bfloat16),
                     preferred_element_type=jnp.float32).astype(jnp.int32)
    earlier = jnp.sum(jnp.where(onehot, counts, 0), axis=1)
    slot_of = (routed * slot + earlier).reshape(tok_dev, top_k)
    places = jnp.arange(rows, dtype=jnp.int32)
    hits = [slot_of[:, k][:, None] == places[None, :] for k in range(top_k)]
    picked = hits[0]
    for hit in hits[1:]:
        picked = picked | hit
    select = picked.astype(jnp.bfloat16)
    offset = lax.axis_index("tp") * quarter
    tok_part = lax.dynamic_slice_in_dim(tokens, offset, quarter, 1)
    cot_part = lax.dynamic_slice_in_dim(cotangent, offset, quarter, 1)
    contract_first = (((0,), (0,)), ((), ()))
    sent_tok = lax.dot_general(select, tok_part, contract_first,
                               preferred_element_type=jnp.float32).astype(jnp.bfloat16)
    sent_cot = lax.dot_general(select, cot_part, contract_first,
                               preferred_element_type=jnp.float32).astype(jnp.bfloat16)
    gate_row = jnp.zeros((rows,), jnp.float32)
    for k in range(top_k):
        gate_row = gate_row + jnp.sum(
            jnp.where(hits[k], gate_weights[:, k].astype(jnp.float32)[:, None], 0.0), axis=0)
    sent_gate = jnp.pad(gate_row.reshape(groups, slot), ((0, 0), (0, lanes - slot)))
    sent_gate = jnp.broadcast_to(
        sent_gate.astype(jnp.bfloat16)[:, None, :], (groups, GATE_ROWS, lanes)
    ).reshape(groups * GATE_ROWS, lanes)
    vmem = pl.BlockSpec(memory_space=pltpu.VMEM)
    hbm = pl.BlockSpec(memory_space=pl.ANY)
    bf, f32 = jnp.bfloat16, jnp.float32
    dma = pltpu.SemaphoreType.DMA
    per = dma((groups,))
    twice = dma((2, groups))
    steps = max(-(-width // 256), -(-ffe // 256))
    back_rows, back_gate, grad_gate_w, grad_up_w, grad_down = pl.pallas_call(
        functools.partial(expert_kernel, groups, slot, quarter),
        out_shape=(
            jax.ShapeDtypeStruct((rows, quarter), bf),
            jax.ShapeDtypeStruct((groups * SUM_ROWS, lanes), f32),
            jax.ShapeDtypeStruct((width, ffe), bf),
            jax.ShapeDtypeStruct((width, ffe), bf),
            jax.ShapeDtypeStruct((ffe, width), bf),
        ),
        in_specs=[vmem, vmem, vmem, hbm, hbm, hbm],
        out_specs=(vmem, vmem, hbm, hbm, hbm),
        scratch_shapes=[
            pltpu.VMEM((rows, width), bf),
            pltpu.VMEM((rows, width), bf),
            pltpu.VMEM((groups * GATE_ROWS, lanes), bf),
            pltpu.VMEM((width, ffe), bf),
            pltpu.VMEM((width, ffe), bf),
            pltpu.VMEM((ffe, width), bf),
            pltpu.VMEM((rows, ffe), f32),
            pltpu.VMEM((rows, ffe), f32),
            pltpu.VMEM((rows, ffe), f32),
            pltpu.VMEM((rows, ffe), bf),
            pltpu.VMEM((rows, 2 * ffe), bf),
            pltpu.VMEM((4, rows, quarter), bf),
            pltpu.VMEM((2, rows, quarter), bf),
            pltpu.VMEM((rows, quarter), bf),
            pltpu.VMEM((rows, quarter), bf),
            pltpu.VMEM((4, groups * SUM_ROWS, lanes), f32),
            pltpu.VMEM((groups * SUM_ROWS, lanes), f32),
            pltpu.VMEM((width, ffe), bf),
            pltpu.VMEM((width, ffe), bf),
            pltpu.VMEM((ffe, width), bf),
            dma((3,)), dma((3,)),
            twice, twice, twice, twice, twice, twice, twice, twice,
            per, per,
            dma((2,)), dma((2,)),
            per, per, per, per,
            dma((3,)), dma((3,)),
            per, per,
            dma((steps, 3)),
        ],
        compiler_params=pltpu.CompilerParams(
            collective_id=0, has_side_effects=True, vmem_limit_bytes=67043328),
    )(sent_tok, sent_cot, sent_gate, w_gate[0], w_up[0], w_down[0])
    grad_tokens = jnp.dot(select, back_rows, preferred_element_type=f32).astype(bf)
    gate_line = back_gate.reshape(groups, SUM_ROWS, lanes)[:, 0, :slot].reshape(rows)
    grad_gates = jnp.stack(
        [jnp.sum(jnp.where(hit, gate_line[None, :], 0.0), axis=1) for hit in hits], axis=1)
    return (grad_tokens, grad_gates, grad_gate_w[None], grad_up_w[None], grad_down[None])


def solution(mesh):
    in_specs = (
        P("ep", None),
        P("ep", None),
        P("ep", None),
        P("ep", None),
        P("ep", None, "tp"),
        P("ep", None, "tp"),
        P("ep", "tp", None),
    )
    out_specs = (
        P("ep", "tp"),
        P("ep", None),
        P("ep", None, "tp"),
        P("ep", None, "tp"),
        P("ep", "tp", None),
    )
    return jax.shard_map(
        on_device, mesh=mesh, in_specs=in_specs, out_specs=out_specs, check_vma=False
    )
```

```python
import functools

import jax
import jax.numpy as jnp
from jax import lax
from jax.experimental import pallas as pl
from jax.experimental.pallas import tpu as pltpu
from jax.sharding import PartitionSpec as P

MESH = pl.DeviceIdType.MESH
LAST = (((1,), (1,)), ((), ()))
FIRST = (((0,), (0,)), ((), ()))
GATE_ROWS = 16
SUM_ROWS = 8


def expert_kernel(groups, slot, quarter,
                  tokens, cots, slots, weights, w_gate, w_up, w_down,
                  back_rows, back_gate, out_gate, out_up, out_down,
                  sent_tok, sent_cot, sent_gate, x_rows, c_rows, gates, wg, wu, wd, gate_pre, up_pre, back, hidden, grads,
                  part, core_got, x_got, total, gate_all, gate_sum,
                  og, ou, od,
                  load_sem, near_sem, first_send, first_recv, core_send, core_recv,
                  x_send, x_recv, second_send, second_recv, gate_send, gate_recv,
                  pair_send, pair_recv, cross_send, cross_recv, home_send, home_recv,
                  sum_send, sum_recv, sumhome_send, sumhome_recv, out_sem):
    me = lax.axis_index("ep")
    t = lax.axis_index("tp")
    core = lax.rem(t, 2)
    side = t // 2
    core_peer = side * 2 + (1 - core)
    x_peer = (1 - side) * 2 + core
    rows = groups * slot
    ffe = wg.shape[1]
    width = wg.shape[0]

    barrier = pltpu.get_barrier_semaphore()

    def greet(d, _):
        pl.semaphore_signal(barrier, inc=1, device_id=(lax.rem(me + d, groups), t),
                            device_id_type=MESH)
        return 0

    loads = [
        pltpu.make_async_copy(w_gate, wg, load_sem.at[0]),
        pltpu.make_async_copy(w_up, wu, load_sem.at[1]),
        pltpu.make_async_copy(w_down, wd, load_sem.at[2]),
    ]
    lax.fori_loop(1, groups, greet, 0)
    for o in range(1, 4):
        pl.semaphore_signal(barrier, inc=1, device_id=(me, lax.rem(t + o, 4)),
                            device_id_type=MESH)
    for load in loads:
        load.start()
    def rblk(ref, s, size=slot):
        return ref.at[pl.ds(pl.multiple_of(s * size, size if size < 16 else 16), size)]

    def blk(ref, s, q):
        return ref.at[pl.ds(pl.multiple_of(s * slot, 16), slot),
                      pl.ds(pl.multiple_of(q * quarter, 128), quarter)]

    def rc(src, dst, ssem, rsem, ep, tp):
        return pltpu.make_async_remote_copy(
            src_ref=src, dst_ref=dst, send_sem=ssem, recv_sem=rsem,
            device_id=(ep, tp), device_id_type=MESH)

    def loop(lo, hi, body):
        def step(d, c):
            body(d)
            return c
        lax.fori_loop(lo, hi, step, 0)

    sent = (sent_tok, sent_cot)
    full = (x_rows, c_rows)

    def hits_of(d):
        base = lax.rem(me + d, groups) * slot
        ids = base + lax.broadcasted_iota(jnp.int32, (slot, slots.shape[1]), 0)
        return [slots[k:k + 1, :] == ids for k in range(weights.shape[0])]

    def any_of(hits):
        found = hits[0]
        for hit in hits[1:]:
            found = found | hit
        return found.astype(jnp.bfloat16)

    def own_cols(ref):
        return ref[:, pl.ds(pl.multiple_of(t * quarter, 128), quarter)]

    def at_block(d, size=slot):
        return pl.ds(pl.multiple_of(d * size, 16), size)

    def pick(src, dst):
        def body(d):
            dst[at_block(d), :] = jnp.dot(
                any_of(hits_of(d)), own_cols(src), preferred_element_type=jnp.float32
            ).astype(jnp.bfloat16)
        return body

    def pick_gate(d, dst):
        row = jnp.zeros((GATE_ROWS, slot), jnp.float32)
        for k, hit in enumerate(hits_of(d)):
            row = row + lax.dot_general(weights[k], hit.astype(jnp.bfloat16), LAST,
                                        preferred_element_type=jnp.float32)
        lanes = gates.shape[1]
        if lanes > slot:
            row = jnp.concatenate(
                [row, jnp.zeros((GATE_ROWS, lanes - slot), jnp.float32)], axis=1)
        dst[at_block(d, GATE_ROWS), :] = row.astype(jnp.bfloat16)

    def first(a, d):
        to = lax.rem(me + d, groups)
        return rc(rblk(sent[a], d), blk(full[a], d, t), first_send.at[a, d],
                  first_recv.at[a, d], to, t)

    def gate_copy(d):
        to = lax.rem(me + d, groups)
        return rc(rblk(sent_gate, d, GATE_ROWS), rblk(gates, d, GATE_ROWS),
                  gate_send.at[d], gate_recv.at[d], to, t)

    def source(d):
        return lax.rem(me - d + groups, groups)

    def to_core(a, d, q):
        return rc(blk(full[a], d, q), blk(full[a], d, q), core_send.at[a, d],
                  core_recv.at[a, d], me, core_peer)

    def to_x(a, d, q):
        return rc(blk(full[a], d, q), blk(full[a], d, q), x_send.at[a, d],
                  x_recv.at[a, d], me, x_peer)

    def to_core_again(a, d, q):
        return rc(blk(full[a], d, q), blk(full[a], d, q), second_send.at[a, d],
                  second_recv.at[a, d], me, core_peer)

    x_core_peer = (1 - side) * 2 + (1 - core)

    loop(1, groups, pick(tokens, sent_tok))
    pl.semaphore_wait(barrier, groups + 2)
    loop(1, groups, lambda d: first(0, d).start())
    loop(1, groups, lambda d: pick_gate(d, sent_gate))
    loop(1, groups, pick(cots, sent_cot))
    loop(1, groups, lambda d: gate_copy(d).start())
    loop(1, groups, lambda d: first(1, d).start())
    pick_gate(0, gates)
    mine = any_of(hits_of(0))
    for src, dst in ((tokens, x_rows), (cots, c_rows)):
        dst[0:slot, :] = jnp.dot(mine, src[...], preferred_element_type=jnp.float32).astype(
            jnp.bfloat16)

    def stage1(a, d):
        first(a, d).wait_recv()
        to_x(a, d, t).start()
        to_core(a, d, t).start()

    def stage2(a, d):
        to_x(a, d, x_peer).wait_recv()
        to_core_again(a, d, x_peer).start()

    def settle(a, lo, hi):
        def body(d):
            to_core(a, d, core_peer).wait_recv()
            to_core_again(a, d, x_core_peer).wait_recv()
        loop(lo, hi, body)

    def both(a):
        def body(d):
            stage1(a, d)
            stage2(a, d - 1)
        return body

    stage1(0, 1)
    loop(2, groups, both(0))
    stage2(0, groups - 1)
    settle(0, 1, groups)
    loads[0].wait()
    loads[1].wait()

    mid = groups // 2
    half = rows // 2
    chunks = []
    at = 0
    while at < ffe:
        chunks.append((at, min(256, ffe - at)))
        at += 256
    pieces = [(w, o, lo, n) for lo, n in chunks for w, o in ((wg, gate_pre), (wu, up_pre))]

    def product(lhs, w, o, lo, n):
        def body(h):
            r = pl.ds(pl.multiple_of(h * half, 16), half)
            o[r, lo:lo + n] = jnp.dot(lhs[r, :], w[:, lo:lo + n],
                                      preferred_element_type=jnp.float32)
        loop(0, 2, body)

    count = len(pieces)
    stage1(1, 1)
    for i, (w, o, lo, n) in enumerate(pieces):
        product(x_rows, w, o, lo, n)
        lower = 2 + i * (mid - 1) // count
        upper = 2 + (i + 1) * (mid - 1) // count
        if upper > lower:
            loop(lower, upper, both(1))
    loop(1, groups, lambda d: gate_copy(d).wait_recv())
    loads[2].wait()

    def back_product(lo, n, h):
        r = pl.ds(h * half, half)
        back[r, lo:lo + n] = lax.dot_general(
            c_rows[r, :], wd[lo:lo + n, :], LAST, preferred_element_type=jnp.float32)

    lanes = gates.shape[1]
    eye = (lax.broadcasted_iota(jnp.int32, (slot, lanes), 0)
           == lax.broadcasted_iota(jnp.int32, (slot, lanes), 1)).astype(jnp.bfloat16)

    def weight_of(s):
        g = gates[pl.ds(pl.multiple_of(s * GATE_ROWS, GATE_ROWS), GATE_ROWS), :]
        return lax.dot_general(eye, g, LAST, preferred_element_type=jnp.float32)[:, 0:1]

    def elementwise(s):
        r = pl.ds(pl.multiple_of(s * slot, 16), slot)
        weight = weight_of(s)
        summed = jnp.zeros((slot, 128), jnp.float32)
        for lo in range(0, ffe, 128):
            g = gate_pre[r, lo:lo + 128]
            u = up_pre[r, lo:lo + 128]
            b = back[r, lo:lo + 128]
            logistic = jax.nn.sigmoid(g)
            act = g * logistic
            h = (act * u).astype(jnp.bfloat16)
            hidden[r, lo:lo + 128] = h
            summed = summed + h.astype(jnp.float32) * b
            gh = weight * b
            grads[r, lo:lo + 128] = (gh * u * logistic * (1.0 + g * (1.0 - logistic))).astype(
                jnp.bfloat16)
            grads[r, ffe + lo:ffe + lo + 128] = (gh * act).astype(jnp.bfloat16)
        padded = jnp.concatenate(
            [summed, jnp.zeros((lanes - slot, 128), jnp.float32)], axis=0) if lanes > slot else summed
        row = jnp.sum(padded.T, axis=0, keepdims=True)
        gate_all[t, pl.ds(pl.multiple_of(s * SUM_ROWS, SUM_ROWS), SUM_ROWS), :] = jnp.broadcast_to(
            row, (SUM_ROWS, lanes))
        cs = c_rows[r, :].astype(jnp.float32) * weight
        c_rows[r, :] = cs.astype(jnp.bfloat16)

    def drain(a, lo, hi):
        def body(d):
            to_core(a, d, t).wait_send()
            to_x(a, d, t).wait_send()
            to_core_again(a, d, x_peer).wait_send()
        loop(lo, hi, body)

    def row_product(q, i, h):
        cols = pl.ds(pl.multiple_of(q * quarter, 128), quarter)
        r = pl.ds(h * half, half)
        value = lax.dot_general(grads[r, 0:ffe], wg[cols, :], LAST,
                                preferred_element_type=jnp.float32)
        value = value + lax.dot_general(grads[r, ffe:2 * ffe], wu[cols, :], LAST,
                                        preferred_element_type=jnp.float32)
        part[i, r, :] = value.astype(jnp.bfloat16)

    def pair(i, h):
        r = pl.ds(h * half, half)
        return rc(part.at[i, r], core_got.at[i, r], pair_send.at[i, h], pair_recv.at[i, h],
                  me, core_peer)

    def cross(d):
        return rc(rblk(part.at[2], d), rblk(x_got, d), cross_send.at[d], cross_recv.at[d],
                  me, x_peer)

    def add_cross(d):
        r = at_block(d)
        part[2, r, :] = (part[2, r, :].astype(jnp.float32)
                         + core_got[0, r, :].astype(jnp.float32)).astype(jnp.bfloat16)
        cross(d).start()

    late = mid + 1
    cuts = [late, late + (groups - late) // 3, late + 2 * (groups - late) // 3, groups]
    for h in range(2):
        lower, upper = h * mid, (h + 1) * mid
        if h == 1:
            stage2(1, groups - 1)
        settle(1, max(1, lower), upper)
        for lo, n in chunks:
            back_product(lo, n, h)
        if h == 0:
            loop(cuts[0], cuts[1], both(1))
        drain(1, max(1, lower), upper)
        loop(lower, upper, elementwise)
        if h == 0:
            loop(cuts[1], cuts[2], both(1))
        row_product(x_core_peer, 0, h)
        pair(0, h).start()
        row_product(x_peer, 2, h)
        pair(0, h).wait_recv()
        loop(lower, upper, add_cross)
        if h == 0:
            loop(cuts[2], cuts[3], both(1))
        if h == 1:
            sums = [rc(gate_all.at[t], gate_all.at[t], sum_send.at[o - 1], sum_recv.at[o - 1],
                       me, lax.rem(t + o, 4)) for o in range(1, 4)]
            for copy in sums:
                copy.start()
        row_product(core_peer, 1, h)
        pair(1, h).start()
        row_product(t, 3, h)
    for copy in sums:
        copy.wait_recv()
    gate_sum[...] = (gate_all[0] + gate_all[1]) + (gate_all[2] + gate_all[3])

    def sum_home(d, land):
        return rc(rblk(gate_sum, d, SUM_ROWS), rblk(back_gate, land, SUM_ROWS),
                  sumhome_send.at[d], sumhome_recv.at[d], source(d), t)

    loop(1, groups, lambda d: sum_home(d, me).start())
    last = pltpu.make_async_copy(rblk(gate_sum, 0, SUM_ROWS), rblk(back_gate, me, SUM_ROWS),
                                 near_sem.at[2])
    last.start()
    for h in range(2):
        pair(1, h).wait_recv()

    def home(d, land):
        return rc(rblk(total, d), rblk(back_rows, land), home_send.at[d], home_recv.at[d],
                  source(d), t)

    def finish(d):
        r = at_block(d)
        cross(d).wait_recv()
        total[r, :] = (part[3, r, :].astype(jnp.float32) + core_got[1, r, :].astype(jnp.float32)
                       + x_got[r, :].astype(jnp.float32)).astype(jnp.bfloat16)

    def finish_send(d):
        finish(d)
        home(d, me).start()

    outs = []
    work = []

    def x_grad(lo, n, i):
        def run():
            left = x_rows[:, lo:lo + n]
            og[lo:lo + n, :] = lax.dot_general(
                left, grads[:, 0:ffe], FIRST, preferred_element_type=jnp.float32
            ).astype(jnp.bfloat16)
            ou[lo:lo + n, :] = lax.dot_general(
                left, grads[:, ffe:2 * ffe], FIRST, preferred_element_type=jnp.float32
            ).astype(jnp.bfloat16)
            for j, (src, dst) in enumerate(((og, out_gate), (ou, out_up))):
                copy = pltpu.make_async_copy(src.at[lo:lo + n], dst.at[lo:lo + n],
                                             out_sem.at[i, j])
                copy.start()
                outs.append(copy)
        return run

    def down_grad(lo, n, i):
        def run():
            od[lo:lo + n, :] = lax.dot_general(
                hidden[:, lo:lo + n], c_rows[...], FIRST, preferred_element_type=jnp.float32
            ).astype(jnp.bfloat16)
            copy = pltpu.make_async_copy(od.at[lo:lo + n], out_down.at[lo:lo + n],
                                         out_sem.at[i, 2])
            copy.start()
            outs.append(copy)
        return run

    step = 256
    for i, lo in enumerate(range(0, width, step)):
        work.append(x_grad(lo, min(step, width - lo), i))
    for i, (lo, n) in enumerate(chunks):
        work.append(down_grad(lo, n, i))
    lead = len(work) - 1
    for i, run in enumerate(work):
        run()
        lower, upper = max(1, 1 + i * (groups - 1) // lead), min(groups, 1 + (i + 1) * (groups - 1) // lead)
        if upper > lower:
            loop(lower, upper, finish_send)
    finish(0)
    own = pltpu.make_async_copy(rblk(total, 0), rblk(back_rows, me), near_sem.at[0])
    own.start()

    loop(1, groups, lambda d: home(d, lax.rem(me + d, groups)).wait_recv())
    loop(1, groups, lambda d: sum_home(d, lax.rem(me + d, groups)).wait_recv())
    own.wait()
    last.wait()
    drain(0, 1, groups)
    for a in range(2):
        loop(1, groups, lambda d, a=a: first(a, d).wait_send())
    loop(1, groups, lambda d: gate_copy(d).wait_send())
    for copy in sums:
        copy.wait_send()
    for i in range(2):
        for h in range(2):
            pair(i, h).wait_send()
    loop(0, groups, lambda d: cross(d).wait_send())
    loop(1, groups, lambda d: home(d, me).wait_send())
    loop(1, groups, lambda d: sum_home(d, me).wait_send())
    for copy in outs:
        copy.wait()


def on_device(tokens, cotangent, gate_weights, routes, w_gate, w_up, w_down):
    tok_dev, width = tokens.shape
    top_k = routes.shape[1]
    groups = lax.axis_size("ep")
    narrow = lax.axis_size("tp")
    pair_count = tok_dev * top_k
    capacity = 3 * top_k * tok_dev // (2 * groups)
    slot = -(-capacity // 16) * 16
    quarter = width // narrow
    ffe = w_gate.shape[2]
    rows = groups * slot
    lanes = -(-slot // 128) * 128
    routed = routes.reshape(pair_count)
    onehot = (routed[:, None] == jnp.arange(groups, dtype=jnp.int32)[None, :])
    before = (jnp.arange(pair_count, dtype=jnp.int32)[:, None]
              > jnp.arange(pair_count, dtype=jnp.int32)[None, :])
    counts = jnp.dot(before.astype(jnp.bfloat16), onehot.astype(jnp.bfloat16),
                     preferred_element_type=jnp.float32).astype(jnp.int32)
    earlier = jnp.sum(jnp.where(onehot, counts, 0), axis=1)
    slot_of = (routed * slot + earlier).reshape(tok_dev, top_k)
    places = jnp.arange(rows, dtype=jnp.int32)
    hits = [slot_of[:, k][:, None] == places[None, :] for k in range(top_k)]
    picked = hits[0]
    for hit in hits[1:]:
        picked = picked | hit
    select = picked.astype(jnp.bfloat16)
    slots = jnp.pad(slot_of.T, ((0, 8 - top_k), (0, 0)), constant_values=-1)
    weights = jnp.broadcast_to(gate_weights.T[:, None, :], (top_k, GATE_ROWS, tok_dev))
    vmem = pl.BlockSpec(memory_space=pltpu.VMEM)
    hbm = pl.BlockSpec(memory_space=pl.ANY)
    bf, f32 = jnp.bfloat16, jnp.float32
    dma = pltpu.SemaphoreType.DMA
    per = dma((groups,))
    twice = dma((2, groups))
    steps = max(-(-width // 256), -(-ffe // 256))
    back_rows, back_gate, grad_gate_w, grad_up_w, grad_down = pl.pallas_call(
        functools.partial(expert_kernel, groups, slot, quarter),
        out_shape=(
            jax.ShapeDtypeStruct((rows, quarter), bf),
            jax.ShapeDtypeStruct((groups * SUM_ROWS, lanes), f32),
            jax.ShapeDtypeStruct((width, ffe), bf),
            jax.ShapeDtypeStruct((width, ffe), bf),
            jax.ShapeDtypeStruct((ffe, width), bf),
        ),
        in_specs=[vmem, vmem, vmem, vmem, hbm, hbm, hbm],
        out_specs=(vmem, vmem, hbm, hbm, hbm),
        scratch_shapes=[
            pltpu.VMEM((rows, quarter), bf),
            pltpu.VMEM((rows, quarter), bf),
            pltpu.VMEM((groups * GATE_ROWS, lanes), bf),
            pltpu.VMEM((rows, width), bf),
            pltpu.VMEM((rows, width), bf),
            pltpu.VMEM((groups * GATE_ROWS, lanes), bf),
            pltpu.VMEM((width, ffe), bf),
            pltpu.VMEM((width, ffe), bf),
            pltpu.VMEM((ffe, width), bf),
            pltpu.VMEM((rows, ffe), f32),
            pltpu.VMEM((rows, ffe), f32),
            pltpu.VMEM((rows, ffe), f32),
            pltpu.VMEM((rows, ffe), bf),
            pltpu.VMEM((rows, 2 * ffe), bf),
            pltpu.VMEM((4, rows, quarter), bf),
            pltpu.VMEM((2, rows, quarter), bf),
            pltpu.VMEM((rows, quarter), bf),
            pltpu.VMEM((rows, quarter), bf),
            pltpu.VMEM((4, groups * SUM_ROWS, lanes), f32),
            pltpu.VMEM((groups * SUM_ROWS, lanes), f32),
            pltpu.VMEM((width, ffe), bf),
            pltpu.VMEM((width, ffe), bf),
            pltpu.VMEM((ffe, width), bf),
            dma((3,)), dma((3,)),
            twice, twice, twice, twice, twice, twice, twice, twice,
            per, per,
            dma((2, 2)), dma((2, 2)),
            per, per, per, per,
            dma((3,)), dma((3,)),
            per, per,
            dma((steps, 3)),
        ],
        compiler_params=pltpu.CompilerParams(
            collective_id=0, has_side_effects=True, vmem_limit_bytes=67043328),
    )(tokens, cotangent, slots, weights, w_gate[0], w_up[0], w_down[0])
    grad_tokens = jnp.dot(select, back_rows, preferred_element_type=f32).astype(bf)
    gate_line = back_gate.reshape(groups, SUM_ROWS, lanes)[:, 0, :slot].reshape(rows)
    grad_gates = jnp.stack(
        [jnp.sum(jnp.where(hit, gate_line[None, :], 0.0), axis=1) for hit in hits], axis=1)
    return (grad_tokens, grad_gates, grad_gate_w[None], grad_up_w[None], grad_down[None])


def solution(mesh):
    in_specs = (
        P("ep", None),
        P("ep", None),
        P("ep", None),
        P("ep", None),
        P("ep", None, "tp"),
        P("ep", None, "tp"),
        P("ep", "tp", None),
    )
    out_specs = (
        P("ep", "tp"),
        P("ep", None),
        P("ep", None, "tp"),
        P("ep", None, "tp"),
        P("ep", "tp", None),
    )
    return jax.shard_map(
        on_device, mesh=mesh, in_specs=in_specs, out_specs=out_specs, check_vma=False
    )
```
